32 devices in a mesh: ep: 4 (over y, x), tp: 8 (over z, core).
Axes of the slice: x: 2, y: 2, z: 4, core: 2. Of those that a mesh axis runs over, the one named last changes fastest.
Arguments:
- tokens: bfloat16 [768, 2048], P('ep'), may hold values from -6 to 6
- cotangent: bfloat16 [768, 2048], P('ep'), may hold values from -6 to 6
- routing: int32 [768, 2], P('ep'), may hold values from 0 to 3, all different within a row; in each aligned block of 192 rows (0 to 191, 192 to 383, ...) at most 192 rows name the same one
- gate_weights: bfloat16 [768, 2], P('ep'), may hold values from 0.19921875 to 1
- gate_proj: bfloat16 [4, 2048, 7168], P('ep', None, 'tp'), may hold values from -0.125 to 0.125
- up_proj: bfloat16 [4, 2048, 7168], P('ep', None, 'tp'), may hold values from -0.125 to 0.125
- down_proj: bfloat16 [4, 7168, 2048], P('ep', 'tp'), may hold values from -0.0625 to 0.0625
Outputs:
- grad_tokens: bfloat16 [768, 2048], P('ep', 'tp')
- grad_gates: float32 [768, 2], P('ep')
- grad_gate_proj: bfloat16 [4, 2048, 7168], P('ep', None, 'tp')
- grad_up_proj: bfloat16 [4, 2048, 7168], P('ep', None, 'tp')
- grad_down_proj: bfloat16 [4, 7168, 2048], P('ep', 'tp')
The draws below stay inside these ranges and needn't reach their ends.
Inputs may be any that keep to these rules, and one draw needn't show every extreme that they name: `routing`: each row names 2 different experts. Within each aligned block of 192 rows no expert is named by more than 192 rows, and in every draw some expert is named by exactly 192 rows of some block.
All inputs are finite; a program needn't handle non-finite values.
Results may differ from the reference program's by a relative error of at most 0.019.
Values may be sent and summed in bfloat16 or wider, within the bound.
A program may use at most 128 MiB of HBM per device.

```python
import math
import jax
import jax.numpy as jnp
import numpy as np
from jax import lax

D = 2048
FF = 7168
TOP_K = 2
TOK_DEV = 192
EXPERTS = 4
CAP = 192
TOKENS = 768
N_EP = 4


def block_scale(stream_key, shape, shards, least, high):
    def one(axis_at, shards_of):
        steps = jax.random.uniform(jax.random.fold_in(jax.random.fold_in(stream_key, 6), axis_at), (shards_of,), jnp.float32, least / len(shards), high / len(shards))
        return jnp.repeat(jnp.exp(steps), shape[axis_at] // shards_of).reshape((-1,) + (1,) * (len(shape) - axis_at - 1))

    level = one(*shards[0])
    for cut in shards[1:]:
        level = level * one(*cut)
    return level


def assign_block(rng, own, number, rows, count, top, limit, slope):
    sequence = jax.random.permutation(rng, count)
    crowded, usual = load_shares(count, rows * top, limit, slope, True), load_shares(count, rows * top, limit, slope, False)
    places = jnp.arange(count)

    def named(sizes, turn):
        used = int((sizes > 0).sum())
        fixed = max(1, used // 4)
        shifted = fixed + (places - fixed + turn * (used - fixed)) % max(1, count - fixed)
        return jnp.zeros((count,), jnp.int32).at[sequence[jnp.where(places < fixed, places, shifted)]].set(jnp.asarray(sizes, jnp.int32))

    sizes = jnp.where(number % 4 == 0, named(crowded, number // 4), named(usual, number - number // 4 - 1))
    mixed = jax.random.permutation(jax.random.fold_in(own, 3), count)
    donor, taker = mixed[0:count // 2 * 2:2], mixed[1:count // 2 * 2:2]
    room = jnp.minimum(sizes[donor] - 1, limit - sizes[taker]) // 2
    room = jnp.where((donor == sequence[0]) | (taker == sequence[0]) | (sizes[taker] == 0), 0, jnp.maximum(room, 0))
    shifted = jax.random.randint(jax.random.fold_in(own, 4), (count // 2,), 0, 1 << 20) % (room + 1)
    sizes = sizes.at[donor].add(-shifted).at[taker].add(shifted)
    items = jnp.searchsorted(jnp.cumsum(sizes), jnp.arange(rows * top), side="right").astype(jnp.int32)
    grid = items.reshape(top, rows).T
    grid = grid[jax.random.permutation(jax.random.fold_in(own, 1), rows)]
    turn = jax.random.randint(jax.random.fold_in(own, 2), (rows, 1), 0, top)
    return jnp.take_along_axis(grid, (jnp.arange(top)[None, :] + turn) % top, axis=1)


def load_shares(number_of, total, most, lean, full):
    portions = [(1 << 20) // math.isqrt(rank ** lean) + 1 for rank in range(1, number_of + 1)]
    largest = most if full else min(most, max(-(-total // number_of), total * portions[0] // sum(portions)))
    least = 1 if total - largest >= number_of - 1 else 0
    counts, surplus = [largest] + [least] * (number_of - 1), total - largest - least * (number_of - 1)
    while surplus > 0:
        free = [i for i in range(1, number_of) if counts[i] < largest] or [i for i in range(1, number_of) if counts[i] < most]
        pool, budget = sum([portions[i] for i in free]), surplus
        for i in free:
            addition = min(most - counts[i], max(1, budget * portions[i] // pool), surplus)
            counts[i] = counts[i] + addition
            surplus = surplus - addition
    return np.array(counts)


def normal_values(rng, extent, deviation, reach, cuts=(), kind=jnp.bfloat16):
    drawn = jax.random.normal(rng, extent, jnp.float32) * deviation
    if len(cuts) > 0:
        drawn = block_scale(rng, extent, cuts, -0.22, 0.18) * drawn
    return jnp.clip(drawn, min=-reach, max=reach).astype(kind)


def setup_inputs(seed: int = 0) -> dict:
    streams_of = jax.random.split(jax.random.key(seed), 8)
    tokens = normal_values(streams_of[0], (TOKENS, D), 1.0, 6.0, ((0, 4),))
    cotangent = normal_values(streams_of[1], (TOKENS, D), 1.0, 6.0, ((0, 4),))
    routing_keys = jax.random.split(jax.random.fold_in(streams_of[2], 1), TOKENS // TOK_DEV)
    routing_turns = jax.random.permutation(jax.random.fold_in(streams_of[2], 3), TOKENS // TOK_DEV)
    routing = jax.vmap(lambda own, number: assign_block(jax.random.fold_in(streams_of[2], 2), own, number, TOK_DEV, EXPERTS, TOP_K, CAP, 1))(routing_keys, routing_turns).reshape((TOKENS, TOP_K))
    gate_weights = jnp.clip(0.19921875 + 0.80078125 * jax.random.uniform(streams_of[3], (TOKENS, TOP_K), jnp.float32) ** block_scale(streams_of[3], (TOKENS, TOP_K), ((0, 4),), -0.2, 0.2), 0.19921875, 1.0).astype(jnp.bfloat16)
    gate_proj = normal_values(streams_of[4], (EXPERTS, D, FF), D ** -0.5, 0.125, ((0, 4), (2, 8)))
    up_proj = normal_values(streams_of[5], (EXPERTS, D, FF), D ** -0.5, 0.125, ((0, 4), (2, 8)))
    down_proj = normal_values(streams_of[6], (EXPERTS, FF, D), FF ** -0.5, 0.0625, ((0, 4), (1, 8)))
    return {"tokens": tokens, "cotangent": cotangent, "routing": routing, "gate_weights": gate_weights, "gate_proj": gate_proj, "up_proj": up_proj, "down_proj": down_proj}


def expert_backward(in_rows, cot_rows, gate_col, w_gate, w_up, w_down):
    gate_pre = jnp.dot(in_rows, w_gate, preferred_element_type=jnp.float32)
    up_value = jnp.dot(in_rows, w_up, preferred_element_type=jnp.float32)
    sigmoid_val = jax.nn.sigmoid(gate_pre)
    active = gate_pre * sigmoid_val
    hidden = (active * up_value).astype(jnp.bfloat16)
    contract_cols = (((1,), (1,)), ((), ()))
    contract_rows = (((0,), (0,)), ((), ()))
    back_hidden = lax.dot_general(cot_rows, w_down, contract_cols, preferred_element_type=jnp.float32)
    gate_part = jnp.sum(hidden.astype(jnp.float32) * back_hidden, axis=1)
    scaled_back = gate_col * back_hidden
    grad_pre = (scaled_back * up_value * sigmoid_val * (1.0 + gate_pre * (1.0 - sigmoid_val))).astype(jnp.bfloat16)
    grad_upval = (scaled_back * active).astype(jnp.bfloat16)
    scaled_cot = (gate_col * cot_rows.astype(jnp.float32)).astype(jnp.bfloat16)
    grad_down = lax.dot_general(hidden, scaled_cot, contract_rows, preferred_element_type=jnp.float32).astype(jnp.bfloat16)
    grad_gate = lax.dot_general(in_rows, grad_pre, contract_rows, preferred_element_type=jnp.float32).astype(jnp.bfloat16)
    grad_upw = lax.dot_general(in_rows, grad_upval, contract_rows, preferred_element_type=jnp.float32).astype(jnp.bfloat16)
    grad_in = lax.dot_general(grad_pre, w_gate, contract_cols, preferred_element_type=jnp.float32)
    grad_in = grad_in + lax.dot_general(grad_upval, w_up, contract_cols, preferred_element_type=jnp.float32)
    return grad_in, gate_part, grad_gate, grad_upw, grad_down


def reference(tokens, cotangent, routing, gate_weights, gate_proj, up_proj, down_proj):
    block_len = TOK_DEV * TOP_K
    flat_routes = routing.reshape(N_EP, block_len).astype(jnp.int32)
    onehot = (flat_routes[:, :, None] == jnp.arange(EXPERTS, dtype=jnp.int32)[None, None, :]).astype(jnp.int32)
    position = (jnp.sum(jnp.cumsum(onehot, axis=1) * onehot, axis=2) - 1).astype(jnp.int32)
    source = jnp.broadcast_to(jnp.arange(N_EP, dtype=jnp.int32)[:, None], (N_EP, block_len))
    global_index = source * block_len + jnp.arange(block_len, dtype=jnp.int32)[None, :]
    slot_owner = jnp.full((EXPERTS, N_EP, CAP), -1, jnp.int32).at[flat_routes, source, position].set(global_index)
    slot_owner = slot_owner.reshape(EXPERTS, N_EP * CAP)
    flat_gates = gate_weights.reshape(-1)

    def one_expert(inputs):
        w_gate, w_up, w_down, owner = inputs
        is_used = owner >= 0
        safe_owner = jnp.where(is_used, owner, 0)
        token_index = safe_owner // TOP_K
        in_rows = jnp.where(is_used[:, None], tokens[token_index], jnp.zeros((), jnp.bfloat16))
        cot_rows = jnp.where(is_used[:, None], cotangent[token_index], jnp.zeros((), jnp.bfloat16))
        gate_col = jnp.where(is_used, flat_gates[safe_owner].astype(jnp.float32), 0.0)[:, None]
        return expert_backward(in_rows, cot_rows, gate_col, w_gate, w_up, w_down)

    grad_in, gate_part, grad_gate, grad_upw, grad_down = lax.map(one_expert, (gate_proj, up_proj, down_proj, slot_owner))
    slot_index = (flat_routes * (N_EP * CAP) + source * CAP + position).reshape(-1)
    picked = grad_in.reshape(EXPERTS * N_EP * CAP, D)[slot_index]
    grad_tokens = jnp.sum(picked.reshape(TOKENS, TOP_K, D), axis=1).astype(jnp.bfloat16)
    grad_gates = gate_part.reshape(-1)[slot_index].reshape(TOKENS, TOP_K)
    return grad_tokens, grad_gates, grad_gate, grad_upw, grad_down
```

```python
import jax
import jax.numpy as jnp
from jax import lax
from jax.sharding import PartitionSpec as P


def expert_backward(in_rows, cot_rows, gate_col, w_gate, w_up, w_down):
    gate_pre = jnp.dot(in_rows, w_gate, preferred_element_type=jnp.float32)
    up_value = jnp.dot(in_rows, w_up, preferred_element_type=jnp.float32)
    sigmoid_val = jax.nn.sigmoid(gate_pre)
    active = gate_pre * sigmoid_val
    hidden = (active * up_value).astype(jnp.bfloat16)
    contract_cols = (((1,), (1,)), ((), ()))
    contract_rows = (((0,), (0,)), ((), ()))
    back_hidden = lax.dot_general(
        cot_rows, w_down, contract_cols, preferred_element_type=jnp.float32
    )
    gate_part = jnp.sum(hidden.astype(jnp.float32) * back_hidden, axis=1)
    scaled_back = gate_col * back_hidden
    grad_pre = (
        scaled_back * up_value * sigmoid_val * (1.0 + gate_pre * (1.0 - sigmoid_val))
    ).astype(jnp.bfloat16)
    grad_upval = (scaled_back * active).astype(jnp.bfloat16)
    scaled_cot = (gate_col * cot_rows.astype(jnp.float32)).astype(jnp.bfloat16)
    grad_down = lax.dot_general(
        hidden, scaled_cot, contract_rows, preferred_element_type=jnp.float32
    ).astype(jnp.bfloat16)
    grad_gate = lax.dot_general(
        in_rows, grad_pre, contract_rows, preferred_element_type=jnp.float32
    ).astype(jnp.bfloat16)
    grad_upw = lax.dot_general(
        in_rows, grad_upval, contract_rows, preferred_element_type=jnp.float32
    ).astype(jnp.bfloat16)
    grad_in = lax.dot_general(grad_pre, w_gate, contract_cols, preferred_element_type=jnp.float32)
    grad_in = grad_in + lax.dot_general(
        grad_upval, w_up, contract_cols, preferred_element_type=jnp.float32
    )
    return (grad_in, gate_part, grad_gate, grad_upw, grad_down)


def slotted(tokens, cotangent, routing, gate_weights, gate_proj, up_proj, down_proj):
    expert_count = lax.axis_size("ep")
    tok_rows, model_width = tokens.shape
    top_k = routing.shape[1]
    capacity = 2 * tok_rows * top_k // expert_count
    flat_routes = routing.reshape(-1)
    onehot = (flat_routes[:, None] == jnp.arange(expert_count, dtype=jnp.int32)[None, :]).astype(
        jnp.int32
    )
    position = jnp.sum(jnp.cumsum(onehot, axis=0) * onehot, axis=1) - 1
    slot_index = flat_routes * capacity + position
    slot_owner = (
        jnp.full((expert_count * capacity,), -1, jnp.int32)
        .at[slot_index]
        .set(jnp.arange(flat_routes.shape[0], dtype=jnp.int32))
    )
    is_used = slot_owner >= 0
    safe_owner = jnp.where(is_used, slot_owner, 0)
    token_index = safe_owner // top_k
    slot_gates = jnp.where(
        is_used, gate_weights.reshape(-1)[safe_owner], jnp.zeros((), jnp.bfloat16)
    )
    slot_gates = slot_gates.reshape(expert_count, capacity)

    def gather_slots(source):
        picked_rows = jnp.where(is_used[:, None], source[token_index], jnp.zeros((), jnp.bfloat16))
        return picked_rows.reshape(expert_count, capacity, source.shape[1])

    col_width = model_width // lax.axis_size("tp")
    col_start = lax.axis_index("tp") * col_width
    token_cols = lax.dynamic_slice_in_dim(tokens, col_start, col_width, 1)
    cot_cols = lax.dynamic_slice_in_dim(cotangent, col_start, col_width, 1)
    rows_part, cots_part, gates_in = (
        lax.all_to_all(gather_slots(token_cols), "ep", split_axis=0, concat_axis=0, tiled=True),
        lax.all_to_all(gather_slots(cot_cols), "ep", split_axis=0, concat_axis=0, tiled=True),
        lax.all_to_all(slot_gates, "ep", split_axis=0, concat_axis=0, tiled=True),
    )
    in_rows, cot_in = (
        lax.all_gather(rows_part, "tp", axis=2, tiled=True),
        lax.all_gather(cots_part, "tp", axis=2, tiled=True),
    )
    slot_count = in_rows.shape[0] * in_rows.shape[1]
    grad_in, gate_part, grad_gate, grad_upw, grad_down = expert_backward(
        in_rows.reshape(slot_count, model_width),
        cot_in.reshape(slot_count, model_width),
        gates_in.reshape(slot_count, 1).astype(jnp.float32),
        gate_proj[0],
        up_proj[0],
        down_proj[0],
    )
    gate_total = lax.psum(gate_part, "tp")
    grad_cols = lax.psum_scatter(
        grad_in.astype(jnp.bfloat16), "tp", scatter_dimension=1, tiled=True
    ).astype(jnp.float32)
    back_rows, back_gates = (
        lax.all_to_all(
            grad_cols.reshape(expert_count, capacity, grad_cols.shape[1]).astype(jnp.bfloat16),
            "ep",
            split_axis=0,
            concat_axis=0,
            tiled=True,
        ).astype(jnp.float32),
        lax.all_to_all(
            gate_total.reshape(expert_count, capacity).astype(jnp.bfloat16),
            "ep",
            split_axis=0,
            concat_axis=0,
            tiled=True,
        ).astype(jnp.float32),
    )
    picked = back_rows.reshape(expert_count * capacity, back_rows.shape[2])[slot_index]
    grad_tokens = jnp.sum(picked.reshape(tok_rows, top_k, picked.shape[1]), axis=1).astype(
        jnp.bfloat16
    )
    grad_gates = back_gates.reshape(-1)[slot_index].reshape(tok_rows, top_k)
    return (grad_tokens, grad_gates, grad_gate[None], grad_upw[None], grad_down[None])


def swap(value, axis, bit):
    size = lax.axis_size(axis)
    return lax.ppermute(value, axis, [(i, i ^ bit) for i in range(size)])


def join(mine, other, bit):
    return jnp.where(
        bit == 0,
        jnp.concatenate([mine, other], axis=-1),
        jnp.concatenate([other, mine], axis=-1),
    )


def dense(tokens, cotangent, routing, gate_weights, gate_proj, up_proj, down_proj):
    f32, bf16 = jnp.float32, jnp.bfloat16
    experts, parts = lax.axis_size("ep"), lax.axis_size("tp")
    rows, width = tokens.shape
    me, t = lax.axis_index("ep"), lax.axis_index("tp")
    core, pair = t % 2, (t // 2) % 2
    both = jnp.stack([tokens, cotangent])
    half = lax.dynamic_slice_in_dim(both, core * (width // 2), width // 2, 2)
    quarter = lax.dynamic_slice_in_dim(
        half, pair * (width // 4), width // 4, 2
    )
    blocks, gates = [both], []
    for j in range(experts):
        own = jnp.sum(
            jnp.where(routing == (me ^ j), gate_weights.astype(f32), 0.0), axis=1, keepdims=True
        ).astype(bf16)
        gates.append(own if j == 0 else swap(own, "ep", j))
    for j in range(1, experts):
        if j == experts - 1:
            got = swap(quarter, "ep", j)
            got = join(got, swap(got, "tp", 2), pair)
        else:
            got = swap(half, "ep", j)
        blocks.append(join(got, swap(got, "tp", 1), core))
    w_gate, w_up, w_down = gate_proj[0], up_proj[0], down_proj[0]
    cols = (((1,), (1,)), ((), ()))
    contract = (((0,), (0,)), ((), ()))
    stage = [[], [], [], []]
    partials, parts_gate = [], []
    for j in range(experts):
        x, cot = blocks[j][0], blocks[j][1]
        g = gates[j].astype(f32)
        pre = jnp.dot(x, w_gate, preferred_element_type=f32)
        up = jnp.dot(x, w_up, preferred_element_type=f32)
        back = lax.dot_general(cot, w_down, cols, preferred_element_type=f32)
        sig = jax.nn.sigmoid(pre)
        act = pre * sig
        hidden = (act * up).astype(bf16)
        parts_gate.append(jnp.sum(hidden.astype(f32) * back, axis=1))
        scaled_back = g * back
        grad_pre = (scaled_back * up * sig * (1.0 + pre * (1.0 - sig))).astype(bf16)
        grad_up = (scaled_back * act).astype(bf16)
        scaled = (g * cot.astype(f32)).astype(bf16)
        for store, value in zip(stage, (hidden, grad_pre, grad_up, scaled)):
            store.append(value)
        total = lax.dot_general(grad_pre, w_gate, cols, preferred_element_type=f32)
        total = total + lax.dot_general(grad_up, w_up, cols, preferred_element_type=f32)
        out = width // parts
        split = total.astype(bf16).reshape(rows, parts // 2, 2, out)
        keep = jnp.where(core == 0, split[:, :, 0], split[:, :, 1])
        give = jnp.where(core == 0, split[:, :, 1], split[:, :, 0])
        mixed = (keep.astype(f32) + swap(give, "tp", 1).astype(f32)).astype(bf16)
        partials.append(mixed if j == 0 else swap(mixed, "ep", j))
    hidden, grad_pre, grad_up, scaled = [jnp.concatenate(v, axis=0) for v in stage]
    x_all = jnp.concatenate([b[0] for b in blocks], axis=0)
    d_gate = lax.dot_general(x_all, grad_pre, contract, preferred_element_type=f32).astype(bf16)
    d_up = lax.dot_general(x_all, grad_up, contract, preferred_element_type=f32).astype(bf16)
    d_down = lax.dot_general(hidden, scaled, contract, preferred_element_type=f32).astype(bf16)

    summed = partials[0].astype(f32)
    for p in partials[1:]:
        summed = summed + p.astype(f32)
    summed = summed.astype(bf16)
    z = t // 2
    final = lax.dynamic_index_in_dim(summed, z, 1, keepdims=False).astype(f32)
    for d in range(1, parts // 2):
        piece = lax.dynamic_index_in_dim(summed, z ^ d, 1, keepdims=False)
        final = final + swap(piece, "tp", 2 * d).astype(f32)
    grad_tokens = final.astype(bf16)

    gate_sum = jnp.stack(parts_gate)
    bit = 1
    while bit < parts:
        gate_sum = gate_sum + swap(gate_sum, "tp", bit)
        bit *= 2
    grad_gates = jnp.zeros(routing.shape, f32)
    for j in range(experts):
        row = gate_sum[j] if j == 0 else swap(gate_sum[j], "ep", j)
        grad_gates = jnp.where(routing == (me ^ j), row[:, None], grad_gates)
    return grad_tokens, grad_gates, d_gate[None], d_up[None], d_down[None]


def local(tokens, cotangent, routing, gate_weights, gate_proj, up_proj, down_proj):
    experts, parts = lax.axis_size("ep"), lax.axis_size("tp")
    capacity = 2 * tokens.shape[0] * routing.shape[1] // experts
    whole = capacity >= tokens.shape[0]
    powers = experts & (experts - 1) == 0 and parts & (parts - 1) == 0 and parts >= 4
    plan = dense if whole and powers else slotted
    return plan(tokens, cotangent, routing, gate_weights, gate_proj, up_proj, down_proj)


def solution(mesh):
    return jax.shard_map(
        local,
        mesh=mesh,
        in_specs=(
            P("ep", None),
            P("ep", None),
            P("ep", None),
            P("ep", None),
            P("ep", None, "tp"),
            P("ep", None, "tp"),
            P("ep", "tp", None),
        ),
        out_specs=(
            P("ep", "tp"),
            P("ep", None),
            P("ep", None, "tp"),
            P("ep", None, "tp"),
            P("ep", "tp", None),
        ),
        check_vma=False,
    )
```

```python
import jax
import jax.numpy as jnp
from jax import lax
from jax.experimental import pallas as pl
from jax.experimental.pallas import tpu as pltpu
from jax.sharding import PartitionSpec as P


def expert_backward(in_rows, cot_rows, gate_col, w_gate, w_up, w_down):
    gate_pre = jnp.dot(in_rows, w_gate, preferred_element_type=jnp.float32)
    up_value = jnp.dot(in_rows, w_up, preferred_element_type=jnp.float32)
    sigmoid_val = jax.nn.sigmoid(gate_pre)
    active = gate_pre * sigmoid_val
    hidden = (active * up_value).astype(jnp.bfloat16)
    contract_cols = (((1,), (1,)), ((), ()))
    contract_rows = (((0,), (0,)), ((), ()))
    back_hidden = lax.dot_general(
        cot_rows, w_down, contract_cols, preferred_element_type=jnp.float32
    )
    gate_part = jnp.sum(hidden.astype(jnp.float32) * back_hidden, axis=1)
    scaled_back = gate_col * back_hidden
    grad_pre = (
        scaled_back * up_value * sigmoid_val * (1.0 + gate_pre * (1.0 - sigmoid_val))
    ).astype(jnp.bfloat16)
    grad_upval = (scaled_back * active).astype(jnp.bfloat16)
    scaled_cot = (gate_col * cot_rows.astype(jnp.float32)).astype(jnp.bfloat16)
    grad_down = lax.dot_general(
        hidden, scaled_cot, contract_rows, preferred_element_type=jnp.float32
    ).astype(jnp.bfloat16)
    grad_gate = lax.dot_general(
        in_rows, grad_pre, contract_rows, preferred_element_type=jnp.float32
    ).astype(jnp.bfloat16)
    grad_upw = lax.dot_general(
        in_rows, grad_upval, contract_rows, preferred_element_type=jnp.float32
    ).astype(jnp.bfloat16)
    grad_in = lax.dot_general(grad_pre, w_gate, contract_cols, preferred_element_type=jnp.float32)
    grad_in = grad_in + lax.dot_general(
        grad_upval, w_up, contract_cols, preferred_element_type=jnp.float32
    )
    return (grad_in, gate_part, grad_gate, grad_upw, grad_down)


def slotted(tokens, cotangent, routing, gate_weights, gate_proj, up_proj, down_proj):
    expert_count = lax.axis_size("ep")
    tok_rows, model_width = tokens.shape
    top_k = routing.shape[1]
    capacity = 2 * tok_rows * top_k // expert_count
    flat_routes = routing.reshape(-1)
    onehot = (flat_routes[:, None] == jnp.arange(expert_count, dtype=jnp.int32)[None, :]).astype(
        jnp.int32
    )
    position = jnp.sum(jnp.cumsum(onehot, axis=0) * onehot, axis=1) - 1
    slot_index = flat_routes * capacity + position
    slot_owner = (
        jnp.full((expert_count * capacity,), -1, jnp.int32)
        .at[slot_index]
        .set(jnp.arange(flat_routes.shape[0], dtype=jnp.int32))
    )
    is_used = slot_owner >= 0
    safe_owner = jnp.where(is_used, slot_owner, 0)
    token_index = safe_owner // top_k
    slot_gates = jnp.where(
        is_used, gate_weights.reshape(-1)[safe_owner], jnp.zeros((), jnp.bfloat16)
    )
    slot_gates = slot_gates.reshape(expert_count, capacity)

    def gather_slots(source):
        picked_rows = jnp.where(is_used[:, None], source[token_index], jnp.zeros((), jnp.bfloat16))
        return picked_rows.reshape(expert_count, capacity, source.shape[1])

    col_width = model_width // lax.axis_size("tp")
    col_start = lax.axis_index("tp") * col_width
    token_cols = lax.dynamic_slice_in_dim(tokens, col_start, col_width, 1)
    cot_cols = lax.dynamic_slice_in_dim(cotangent, col_start, col_width, 1)
    rows_part, cots_part, gates_in = (
        lax.all_to_all(gather_slots(token_cols), "ep", split_axis=0, concat_axis=0, tiled=True),
        lax.all_to_all(gather_slots(cot_cols), "ep", split_axis=0, concat_axis=0, tiled=True),
        lax.all_to_all(slot_gates, "ep", split_axis=0, concat_axis=0, tiled=True),
    )
    in_rows, cot_in = (
        lax.all_gather(rows_part, "tp", axis=2, tiled=True),
        lax.all_gather(cots_part, "tp", axis=2, tiled=True),
    )
    slot_count = in_rows.shape[0] * in_rows.shape[1]
    grad_in, gate_part, grad_gate, grad_upw, grad_down = expert_backward(
        in_rows.reshape(slot_count, model_width),
        cot_in.reshape(slot_count, model_width),
        gates_in.reshape(slot_count, 1).astype(jnp.float32),
        gate_proj[0],
        up_proj[0],
        down_proj[0],
    )
    gate_total = lax.psum(gate_part, "tp")
    grad_cols = lax.psum_scatter(
        grad_in.astype(jnp.bfloat16), "tp", scatter_dimension=1, tiled=True
    ).astype(jnp.float32)
    back_rows, back_gates = (
        lax.all_to_all(
            grad_cols.reshape(expert_count, capacity, grad_cols.shape[1]).astype(jnp.bfloat16),
            "ep",
            split_axis=0,
            concat_axis=0,
            tiled=True,
        ).astype(jnp.float32),
        lax.all_to_all(
            gate_total.reshape(expert_count, capacity).astype(jnp.bfloat16),
            "ep",
            split_axis=0,
            concat_axis=0,
            tiled=True,
        ).astype(jnp.float32),
    )
    picked = back_rows.reshape(expert_count * capacity, back_rows.shape[2])[slot_index]
    grad_tokens = jnp.sum(picked.reshape(tok_rows, top_k, picked.shape[1]), axis=1).astype(
        jnp.bfloat16
    )
    grad_gates = back_gates.reshape(-1)[slot_index].reshape(tok_rows, top_k)
    return (grad_tokens, grad_gates, grad_gate[None], grad_upw[None], grad_down[None])


MESH = pl.DeviceIdType.MESH


def flip(index, mask):
    if mask & 1:
        index = index + 1 - 2 * (index % 2)
    if mask & 2:
        index = index + 2 - 4 * ((index // 2) % 2)
    if mask & 4:
        index = index + 4 - 8 * ((index // 4) % 2)
    return index


class Copies:
    def __init__(self, send_sem, recv_sem):
        self.send_sem, self.recv_sem, self.made = send_sem, recv_sem, []

    def send(self, src, dst, ep, tp):
        n = len(self.made)
        copy = pltpu.make_async_remote_copy(
            src_ref=src,
            dst_ref=dst,
            send_sem=self.send_sem.at[n],
            recv_sem=self.recv_sem.at[n],
            device_id=(ep, tp),
            device_id_type=MESH,
        )
        copy.start()
        self.made.append(copy)
        return copy

    def finish(self):
        for copy in self.made:
            copy.wait_send()


def gather_kernel(tok, cot, gate, tok_out, cot_out, gate_out, send_sem, recv_sem, own_sem):
    me, t = lax.axis_index("ep"), lax.axis_index("tp")
    width = tok.shape[1]
    eighth = width // 8
    quarter = 2 * eighth
    q, far = t % 4, flip(t % 4, 2)

    def cols(start, size):
        return pl.ds(pl.multiple_of(start, 128), size)

    low, high = cols(quarter * q, eighth), cols(quarter * q + eighth, eighth)
    full = cols(quarter * q, quarter)
    far_low, far_high = cols(quarter * far, eighth), cols(quarter * far + eighth, eighth)
    far_full = cols(quarter * far, quarter)
    pairs = ((tok, tok_out), (cot, cot_out))
    own = [
        pltpu.make_async_copy(src, dst.at[0], own_sem.at[a]) for a, (src, dst) in enumerate(pairs)
    ]
    for copy in own:
        copy.start()
    do = Copies(send_sem, recv_sem)
    gates = [do.send(gate.at[j], gate_out.at[j], flip(me, j), t) for j in (1, 2, 3)]
    relayed, direct = [], []
    for src, dst in pairs:
        for j, where in ((3, full), (1, high), (2, high)):
            copy = do.send(src.at[:, where], dst.at[j, :, where], flip(me, j), t)
            relayed.append((copy, dst, j, where))
    for src, dst in pairs:
        for where in (low, far_low):
            for j in (1, 2):
                copy = do.send(src.at[:, where], dst.at[j, :, where], flip(me, j), t)
                direct.append((copy, dst, j, where))
    last = []
    for copy, dst, j, where in relayed:
        copy.wait_recv()
        piece = dst.at[j, :, where]
        moved = do.send(piece, piece, me, flip(t, 2))
        direct.append((moved, dst, j, far_full if j == 3 else far_high))
        last.append(do.send(piece, piece, me, flip(t, 1)))
    for copy, dst, j, where in direct:
        copy.wait_recv()
        piece = dst.at[j, :, where]
        last.append(do.send(piece, piece, me, flip(t, 1)))
    for copy in last + gates:
        copy.wait_recv()
    do.finish()
    gate_out[0] = gate[0]
    for copy in own:
        copy.wait()


def gather(tokens, cotangent, gate):
    experts = lax.axis_size("ep")
    shape = jax.ShapeDtypeStruct((experts,) + tokens.shape, tokens.dtype)
    vmem = pl.BlockSpec(memory_space=pltpu.VMEM)
    return pl.pallas_call(
        gather_kernel,
        out_shape=[shape, shape, jax.ShapeDtypeStruct(gate.shape, gate.dtype)],
        in_specs=[vmem] * 3,
        out_specs=[vmem] * 3,
        scratch_shapes=[
            pltpu.SemaphoreType.DMA((43,)),
            pltpu.SemaphoreType.DMA((43,)),
            pltpu.SemaphoreType.DMA((2,)),
        ],
        compiler_params=pltpu.CompilerParams(has_side_effects=True),
    )(tokens, cotangent, gate)


def reduce_kernel(part, gate, out, gate_out, r1, m, r2, s, r3, rg, g, send_sem, recv_sem):
    me, t = lax.axis_index("ep"), lax.axis_index("tp")
    core, z = t % 2, t // 2
    size = out.shape[1]
    other = flip(t, 1)
    order = (3, 2, 1, 0)
    blocks = (3, 1, 2, 0)
    f32 = jnp.float32

    def cols(d, which):
        return pl.ds(pl.multiple_of((2 * flip(z, d) + which) * size, 128), size)

    do = Copies(send_sem, recv_sem)
    first = {}
    for d in order:
        for j in blocks:
            first[d, j] = do.send(part.at[j, :, cols(d, 1 - core)], r1.at[d, j], me, other)
        if d == 3:
            stage = do.send(gate, rg.at[0], me, other)
    second = {}
    for n, d in enumerate(order):
        for j in blocks:
            first[d, j].wait_recv()
            mine = part[j, :, cols(d, core)].astype(f32)
            m[d, j] = (mine + r1[d, j].astype(f32)).astype(m.dtype)
            if j > 0:
                second[d, j] = do.send(m.at[d, j], r2.at[d, j], flip(me, j), t)
        if n < 3:
            stage.wait_recv()
            g[n] = (gate[...] if n == 0 else g[n - 1]) + rg[n]
            if n < 2:
                stage = do.send(g.at[n], rg.at[n + 1], me, flip(t, 2 << n))
    gates = [do.send(g.at[2, j], gate_out.at[j], flip(me, j), t) for j in (1, 2, 3)]
    third = {}
    for d in order:
        total = m[d, 0].astype(f32)
        for j in (1, 2, 3):
            second[d, j].wait_recv()
            total = total + r2[d, j].astype(f32)
        if d:
            s[d] = total.astype(s.dtype)
            third[d] = do.send(s.at[d], r3.at[d], me, flip(t, 2 * d))
    for d in (3, 2, 1):
        third[d].wait_recv()
        total = total + r3[d].astype(f32)
    out[...] = total.astype(out.dtype)
    for copy in gates:
        copy.wait_recv()
    do.finish()
    gate_out[0] = g[2, 0]


def reduce(part, gate):
    experts, parts = lax.axis_size("ep"), lax.axis_size("tp")
    rows, size = part.shape[1], part.shape[2] // parts
    vmem = pl.BlockSpec(memory_space=pltpu.VMEM)
    slots = parts // 2
    tile = pltpu.VMEM((slots, experts, rows, size), part.dtype)
    return pl.pallas_call(
        reduce_kernel,
        out_shape=[
            jax.ShapeDtypeStruct((rows, size), part.dtype),
            jax.ShapeDtypeStruct(gate.shape, gate.dtype),
        ],
        in_specs=[vmem] * 2,
        out_specs=[vmem] * 2,
        scratch_shapes=[
            tile,
            tile,
            tile,
            pltpu.VMEM((slots, rows, size), part.dtype),
            pltpu.VMEM((slots, rows, size), part.dtype),
            pltpu.VMEM((3,) + gate.shape, gate.dtype),
            pltpu.VMEM((3,) + gate.shape, gate.dtype),
            pltpu.SemaphoreType.DMA((37,)),
            pltpu.SemaphoreType.DMA((37,)),
        ],
        compiler_params=pltpu.CompilerParams(has_side_effects=True),
    )(part, gate)


def tiles(values):
    rows = values.shape[1]
    padded = jnp.pad(values, ((0, 0), (0, -rows % 128)))
    return jnp.broadcast_to(padded[:, None, :], (padded.shape[0], 8, padded.shape[1]))


def dense(tokens, cotangent, routing, gate_weights, gate_proj, up_proj, down_proj):
    f32, bf16 = jnp.float32, jnp.bfloat16
    experts = lax.axis_size("ep")
    rows, width = tokens.shape
    me = lax.axis_index("ep")
    named = [routing == (me ^ j) for j in range(experts)]
    weights = jnp.stack(
        [jnp.sum(jnp.where(n, gate_weights.astype(f32), 0.0), axis=1) for n in named]
    )
    x_all, cot_all, g_all = gather(tokens, cotangent, tiles(weights))
    x, cot = x_all.reshape(-1, width), cot_all.reshape(-1, width)
    g = g_all[:, 0, :rows].reshape(-1, 1)
    grad_in, gate_part, d_gate, d_up, d_down = expert_backward(
        x, cot, g, gate_proj[0], up_proj[0], down_proj[0]
    )
    grad_tokens, gate_sum = reduce(
        grad_in.astype(bf16).reshape(experts, rows, width),
        tiles(gate_part.reshape(experts, rows)),
    )
    grad_gates = jnp.zeros(routing.shape, f32)
    for j in range(experts):
        grad_gates = jnp.where(named[j], gate_sum[j, 0, :rows][:, None], grad_gates)
    return grad_tokens, grad_gates, d_gate[None], d_up[None], d_down[None]


def local(tokens, cotangent, routing, gate_weights, gate_proj, up_proj, down_proj):
    experts, parts = lax.axis_size("ep"), lax.axis_size("tp")
    capacity = 2 * tokens.shape[0] * routing.shape[1] // experts
    fits = experts == 4 and parts == 8 and tokens.shape[1] % 1024 == 0
    plan = dense if capacity >= tokens.shape[0] and fits else slotted
    return plan(tokens, cotangent, routing, gate_weights, gate_proj, up_proj, down_proj)


def solution(mesh):
    return jax.shard_map(
        local,
        mesh=mesh,
        in_specs=(
            P("ep", None),
            P("ep", None),
            P("ep", None),
            P("ep", None),
            P("ep", None, "tp"),
            P("ep", None, "tp"),
            P("ep", "tp", None),
        ),
        out_specs=(
            P("ep", "tp"),
            P("ep", None),
            P("ep", None, "tp"),
            P("ep", None, "tp"),
            P("ep", "tp", None),
        ),
        check_vma=False,
    )
```

```python
import jax
import jax.numpy as jnp
from jax import lax
from jax.experimental import pallas as pl
from jax.experimental.pallas import tpu as pltpu
from jax.sharding import PartitionSpec as P


def expert_backward(in_rows, cot_rows, gate_col, w_gate, w_up, w_down):
    gate_pre = jnp.dot(in_rows, w_gate, preferred_element_type=jnp.float32)
    up_value = jnp.dot(in_rows, w_up, preferred_element_type=jnp.float32)
    sigmoid_val = jax.nn.sigmoid(gate_pre)
    active = gate_pre * sigmoid_val
    hidden = (active * up_value).astype(jnp.bfloat16)
    contract_cols = (((1,), (1,)), ((), ()))
    contract_rows = (((0,), (0,)), ((), ()))
    back_hidden = lax.dot_general(
        cot_rows, w_down, contract_cols, preferred_element_type=jnp.float32
    )
    gate_part = jnp.sum(hidden.astype(jnp.float32) * back_hidden, axis=1)
    scaled_back = gate_col * back_hidden
    grad_pre = (
        scaled_back * up_value * sigmoid_val * (1.0 + gate_pre * (1.0 - sigmoid_val))
    ).astype(jnp.bfloat16)
    grad_upval = (scaled_back * active).astype(jnp.bfloat16)
    scaled_cot = (gate_col * cot_rows.astype(jnp.float32)).astype(jnp.bfloat16)
    grad_down = lax.dot_general(
        hidden, scaled_cot, contract_rows, preferred_element_type=jnp.float32
    ).astype(jnp.bfloat16)
    grad_gate = lax.dot_general(
        in_rows, grad_pre, contract_rows, preferred_element_type=jnp.float32
    ).astype(jnp.bfloat16)
    grad_upw = lax.dot_general(
        in_rows, grad_upval, contract_rows, preferred_element_type=jnp.float32
    ).astype(jnp.bfloat16)
    grad_in = lax.dot_general(grad_pre, w_gate, contract_cols, preferred_element_type=jnp.float32)
    grad_in = grad_in + lax.dot_general(
        grad_upval, w_up, contract_cols, preferred_element_type=jnp.float32
    )
    return (grad_in, gate_part, grad_gate, grad_upw, grad_down)


def slotted(tokens, cotangent, routing, gate_weights, gate_proj, up_proj, down_proj):
    expert_count = lax.axis_size("ep")
    tok_rows, model_width = tokens.shape
    top_k = routing.shape[1]
    capacity = 2 * tok_rows * top_k // expert_count
    flat_routes = routing.reshape(-1)
    onehot = (flat_routes[:, None] == jnp.arange(expert_count, dtype=jnp.int32)[None, :]).astype(
        jnp.int32
    )
    position = jnp.sum(jnp.cumsum(onehot, axis=0) * onehot, axis=1) - 1
    slot_index = flat_routes * capacity + position
    slot_owner = (
        jnp.full((expert_count * capacity,), -1, jnp.int32)
        .at[slot_index]
        .set(jnp.arange(flat_routes.shape[0], dtype=jnp.int32))
    )
    is_used = slot_owner >= 0
    safe_owner = jnp.where(is_used, slot_owner, 0)
    token_index = safe_owner // top_k
    slot_gates = jnp.where(
        is_used, gate_weights.reshape(-1)[safe_owner], jnp.zeros((), jnp.bfloat16)
    )
    slot_gates = slot_gates.reshape(expert_count, capacity)

    def gather_slots(source):
        picked_rows = jnp.where(is_used[:, None], source[token_index], jnp.zeros((), jnp.bfloat16))
        return picked_rows.reshape(expert_count, capacity, source.shape[1])

    col_width = model_width // lax.axis_size("tp")
    col_start = lax.axis_index("tp") * col_width
    token_cols = lax.dynamic_slice_in_dim(tokens, col_start, col_width, 1)
    cot_cols = lax.dynamic_slice_in_dim(cotangent, col_start, col_width, 1)
    rows_part, cots_part, gates_in = (
        lax.all_to_all(gather_slots(token_cols), "ep", split_axis=0, concat_axis=0, tiled=True),
        lax.all_to_all(gather_slots(cot_cols), "ep", split_axis=0, concat_axis=0, tiled=True),
        lax.all_to_all(slot_gates, "ep", split_axis=0, concat_axis=0, tiled=True),
    )
    in_rows, cot_in = (
        lax.all_gather(rows_part, "tp", axis=2, tiled=True),
        lax.all_gather(cots_part, "tp", axis=2, tiled=True),
    )
    slot_count = in_rows.shape[0] * in_rows.shape[1]
    grad_in, gate_part, grad_gate, grad_upw, grad_down = expert_backward(
        in_rows.reshape(slot_count, model_width),
        cot_in.reshape(slot_count, model_width),
        gates_in.reshape(slot_count, 1).astype(jnp.float32),
        gate_proj[0],
        up_proj[0],
        down_proj[0],
    )
    gate_total = lax.psum(gate_part, "tp")
    grad_cols = lax.psum_scatter(
        grad_in.astype(jnp.bfloat16), "tp", scatter_dimension=1, tiled=True
    ).astype(jnp.float32)
    back_rows, back_gates = (
        lax.all_to_all(
            grad_cols.reshape(expert_count, capacity, grad_cols.shape[1]).astype(jnp.bfloat16),
            "ep",
            split_axis=0,
            concat_axis=0,
            tiled=True,
        ).astype(jnp.float32),
        lax.all_to_all(
            gate_total.reshape(expert_count, capacity).astype(jnp.bfloat16),
            "ep",
            split_axis=0,
            concat_axis=0,
            tiled=True,
        ).astype(jnp.float32),
    )
    picked = back_rows.reshape(expert_count * capacity, back_rows.shape[2])[slot_index]
    grad_tokens = jnp.sum(picked.reshape(tok_rows, top_k, picked.shape[1]), axis=1).astype(
        jnp.bfloat16
    )
    grad_gates = back_gates.reshape(-1)[slot_index].reshape(tok_rows, top_k)
    return (grad_tokens, grad_gates, grad_gate[None], grad_upw[None], grad_down[None])


MESH = pl.DeviceIdType.MESH


def flip(index, mask):
    if mask & 1:
        index = index + 1 - 2 * (index % 2)
    if mask & 2:
        index = index + 2 - 4 * ((index // 2) % 2)
    if mask & 4:
        index = index + 4 - 8 * ((index // 4) % 2)
    return index


class Copies:
    def __init__(self, send_sem, recv_sem):
        self.send_sem, self.recv_sem, self.made = send_sem, recv_sem, []

    def send(self, src, dst, ep, tp):
        n = len(self.made)
        copy = pltpu.make_async_remote_copy(
            src_ref=src,
            dst_ref=dst,
            send_sem=self.send_sem.at[n],
            recv_sem=self.recv_sem.at[n],
            device_id=(ep, tp),
            device_id_type=MESH,
        )
        copy.start()
        self.made.append(copy)
        return copy

    def finish(self):
        for copy in self.made:
            copy.wait_send()


def gather_kernel(tok, cot, gate, tok_out, cot_out, gate_out, send_sem, recv_sem, own_sem):
    me, t = lax.axis_index("ep"), lax.axis_index("tp")
    width = tok.shape[1]
    eighth = width // 8
    quarter = 2 * eighth
    q, far = t % 4, flip(t % 4, 2)

    def cols(start, size):
        return pl.ds(pl.multiple_of(start, 128), size)

    low, high = cols(quarter * q, eighth), cols(quarter * q + eighth, eighth)
    far_low, far_high = cols(quarter * far, eighth), cols(quarter * far + eighth, eighth)
    pairs = ((tok, tok_out), (cot, cot_out))
    own = [
        pltpu.make_async_copy(src, dst.at[0], own_sem.at[a]) for a, (src, dst) in enumerate(pairs)
    ]
    for copy in own:
        copy.start()
    do = Copies(send_sem, recv_sem)
    gates = [do.send(gate.at[j], gate_out.at[j], flip(me, j), t) for j in (1, 2, 3)]
    relayed, direct = [], []
    for src, dst in pairs:
        for j in (3, 1, 2):
            copy = do.send(src.at[:, high], dst.at[j, :, high], flip(me, j), t)
            relayed.append((copy, dst, j, high))
    for src, dst in pairs:
        for where in (low, far_low):
            for j in (3, 1, 2):
                copy = do.send(src.at[:, where], dst.at[j, :, where], flip(me, j), t)
                direct.append((copy, dst, j, where))
    last = []
    for copy, dst, j, where in relayed:
        copy.wait_recv()
        piece = dst.at[j, :, where]
        moved = do.send(piece, piece, me, flip(t, 2))
        direct.append((moved, dst, j, far_high))
        last.append(do.send(piece, piece, me, flip(t, 1)))
    for copy, dst, j, where in direct:
        copy.wait_recv()
        piece = dst.at[j, :, where]
        last.append(do.send(piece, piece, me, flip(t, 1)))
    for copy in last + gates:
        copy.wait_recv()
    do.finish()
    gate_out[0] = gate[0]
    for copy in own:
        copy.wait()


def gather(tokens, cotangent, gate):
    experts = lax.axis_size("ep")
    shape = jax.ShapeDtypeStruct((experts,) + tokens.shape, tokens.dtype)
    vmem = pl.BlockSpec(memory_space=pltpu.VMEM)
    return pl.pallas_call(
        gather_kernel,
        out_shape=[shape, shape, jax.ShapeDtypeStruct(gate.shape, gate.dtype)],
        in_specs=[vmem] * 3,
        out_specs=[vmem] * 3,
        scratch_shapes=[
            pltpu.SemaphoreType.DMA((51,)),
            pltpu.SemaphoreType.DMA((51,)),
            pltpu.SemaphoreType.DMA((2,)),
        ],
        compiler_params=pltpu.CompilerParams(has_side_effects=True),
    )(tokens, cotangent, gate)


def reduce_kernel(part, gate, out, gate_out, r1, m, r2, s, r3, rg, g, send_sem, recv_sem):
    me, t = lax.axis_index("ep"), lax.axis_index("tp")
    core, z = t % 2, t // 2
    size = out.shape[1]
    other = flip(t, 1)
    order = (3, 2, 1, 0)
    blocks = (3, 1, 2, 0)
    f32 = jnp.float32

    def cols(d, which):
        return pl.ds(pl.multiple_of((2 * flip(z, d) + which) * size, 128), size)

    do = Copies(send_sem, recv_sem)
    first = {}
    for d in order:
        for j in blocks:
            first[d, j] = do.send(part.at[j, :, cols(d, 1 - core)], r1.at[d, j], me, other)
        if d == 3:
            stage = do.send(gate, rg.at[0], me, other)
    second = {}
    for n, d in enumerate(order):
        for j in blocks:
            first[d, j].wait_recv()
            mine = part[j, :, cols(d, core)].astype(f32)
            m[d, j] = (mine + r1[d, j].astype(f32)).astype(m.dtype)
            if j > 0:
                second[d, j] = do.send(m.at[d, j], r2.at[d, j], flip(me, j), t)
        if n < 3:
            stage.wait_recv()
            g[n] = (gate[...] if n == 0 else g[n - 1]) + rg[n]
            if n < 2:
                stage = do.send(g.at[n], rg.at[n + 1], me, flip(t, 2 << n))
    gates = [do.send(g.at[2, j], gate_out.at[j], flip(me, j), t) for j in (1, 2, 3)]
    third = {}
    for d in order:
        total = m[d, 0].astype(f32)
        for j in (1, 2, 3):
            second[d, j].wait_recv()
            total = total + r2[d, j].astype(f32)
        if d:
            s[d] = total.astype(s.dtype)
            third[d] = do.send(s.at[d], r3.at[d], me, flip(t, 2 * d))
    for d in (3, 2, 1):
        third[d].wait_recv()
        total = total + r3[d].astype(f32)
    out[...] = total.astype(out.dtype)
    for copy in gates:
        copy.wait_recv()
    do.finish()
    gate_out[0] = g[2, 0]


def reduce(part, gate):
    experts, parts = lax.axis_size("ep"), lax.axis_size("tp")
    rows, size = part.shape[1], part.shape[2] // parts
    vmem = pl.BlockSpec(memory_space=pltpu.VMEM)
    slots = parts // 2
    tile = pltpu.VMEM((slots, experts, rows, size), part.dtype)
    return pl.pallas_call(
        reduce_kernel,
        out_shape=[
            jax.ShapeDtypeStruct((rows, size), part.dtype),
            jax.ShapeDtypeStruct(gate.shape, gate.dtype),
        ],
        in_specs=[vmem] * 2,
        out_specs=[vmem] * 2,
        scratch_shapes=[
            tile,
            tile,
            tile,
            pltpu.VMEM((slots, rows, size), part.dtype),
            pltpu.VMEM((slots, rows, size), part.dtype),
            pltpu.VMEM((3,) + gate.shape, gate.dtype),
            pltpu.VMEM((3,) + gate.shape, gate.dtype),
            pltpu.SemaphoreType.DMA((37,)),
            pltpu.SemaphoreType.DMA((37,)),
        ],
        compiler_params=pltpu.CompilerParams(has_side_effects=True),
    )(part, gate)


def tiles(values):
    rows = values.shape[1]
    padded = jnp.pad(values, ((0, 0), (0, -rows % 128)))
    return jnp.broadcast_to(padded[:, None, :], (padded.shape[0], 8, padded.shape[1]))


def dense(tokens, cotangent, routing, gate_weights, gate_proj, up_proj, down_proj):
    f32, bf16 = jnp.float32, jnp.bfloat16
    experts = lax.axis_size("ep")
    rows, width = tokens.shape
    me = lax.axis_index("ep")
    named = [routing == (me ^ j) for j in range(experts)]
    weights = jnp.stack(
        [jnp.sum(jnp.where(n, gate_weights.astype(f32), 0.0), axis=1) for n in named]
    )
    x_all, cot_all, g_all = gather(tokens, cotangent, tiles(weights))
    x, cot = x_all.reshape(-1, width), cot_all.reshape(-1, width)
    g = g_all[:, 0, :rows].reshape(-1, 1)
    grad_in, gate_part, d_gate, d_up, d_down = expert_backward(
        x, cot, g, gate_proj[0], up_proj[0], down_proj[0]
    )
    grad_tokens, gate_sum = reduce(
        grad_in.astype(bf16).reshape(experts, rows, width),
        tiles(gate_part.reshape(experts, rows)),
    )
    grad_gates = jnp.zeros(routing.shape, f32)
    for j in range(experts):
        grad_gates = jnp.where(named[j], gate_sum[j, 0, :rows][:, None], grad_gates)
    return grad_tokens, grad_gates, d_gate[None], d_up[None], d_down[None]


def local(tokens, cotangent, routing, gate_weights, gate_proj, up_proj, down_proj):
    experts, parts = lax.axis_size("ep"), lax.axis_size("tp")
    capacity = 2 * tokens.shape[0] * routing.shape[1] // experts
    fits = experts == 4 and parts == 8 and tokens.shape[1] % 1024 == 0
    plan = dense if capacity >= tokens.shape[0] and fits else slotted
    return plan(tokens, cotangent, routing, gate_weights, gate_proj, up_proj, down_proj)


def solution(mesh):
    return jax.shard_map(
        local,
        mesh=mesh,
        in_specs=(
            P("ep", None),
            P("ep", None),
            P("ep", None),
            P("ep", None),
            P("ep", None, "tp"),
            P("ep", None, "tp"),
            P("ep", "tp", None),
        ),
        out_specs=(
            P("ep", "tp"),
            P("ep", None),
            P("ep", None, "tp"),
            P("ep", None, "tp"),
            P("ep", "tp", None),
        ),
        check_vma=False,
    )
```

```python
import jax
import jax.numpy as jnp
from jax import lax
from jax.experimental import pallas as pl
from jax.experimental.pallas import tpu as pltpu
from jax.sharding import PartitionSpec as P


def expert_backward(in_rows, cot_rows, gate_col, w_gate, w_up, w_down):
    gate_pre = jnp.dot(in_rows, w_gate, preferred_element_type=jnp.float32)
    up_value = jnp.dot(in_rows, w_up, preferred_element_type=jnp.float32)
    sigmoid_val = jax.nn.sigmoid(gate_pre)
    active = gate_pre * sigmoid_val
    hidden = (active * up_value).astype(jnp.bfloat16)
    contract_cols = (((1,), (1,)), ((), ()))
    contract_rows = (((0,), (0,)), ((), ()))
    back_hidden = lax.dot_general(
        cot_rows, w_down, contract_cols, preferred_element_type=jnp.float32
    )
    gate_part = jnp.sum(hidden.astype(jnp.float32) * back_hidden, axis=1)
    scaled_back = gate_col * back_hidden
    grad_pre = (
        scaled_back * up_value * sigmoid_val * (1.0 + gate_pre * (1.0 - sigmoid_val))
    ).astype(jnp.bfloat16)
    grad_upval = (scaled_back * active).astype(jnp.bfloat16)
    scaled_cot = (gate_col * cot_rows.astype(jnp.float32)).astype(jnp.bfloat16)
    grad_down = lax.dot_general(
        hidden, scaled_cot, contract_rows, preferred_element_type=jnp.float32
    ).astype(jnp.bfloat16)
    grad_gate = lax.dot_general(
        in_rows, grad_pre, contract_rows, preferred_element_type=jnp.float32
    ).astype(jnp.bfloat16)
    grad_upw = lax.dot_general(
        in_rows, grad_upval, contract_rows, preferred_element_type=jnp.float32
    ).astype(jnp.bfloat16)
    grad_in = lax.dot_general(grad_pre, w_gate, contract_cols, preferred_element_type=jnp.float32)
    grad_in = grad_in + lax.dot_general(
        grad_upval, w_up, contract_cols, preferred_element_type=jnp.float32
    )
    return (grad_in, gate_part, grad_gate, grad_upw, grad_down)


def slotted(tokens, cotangent, routing, gate_weights, gate_proj, up_proj, down_proj):
    expert_count = lax.axis_size("ep")
    tok_rows, model_width = tokens.shape
    top_k = routing.shape[1]
    capacity = 2 * tok_rows * top_k // expert_count
    flat_routes = routing.reshape(-1)
    onehot = (flat_routes[:, None] == jnp.arange(expert_count, dtype=jnp.int32)[None, :]).astype(
        jnp.int32
    )
    position = jnp.sum(jnp.cumsum(onehot, axis=0) * onehot, axis=1) - 1
    slot_index = flat_routes * capacity + position
    slot_owner = (
        jnp.full((expert_count * capacity,), -1, jnp.int32)
        .at[slot_index]
        .set(jnp.arange(flat_routes.shape[0], dtype=jnp.int32))
    )
    is_used = slot_owner >= 0
    safe_owner = jnp.where(is_used, slot_owner, 0)
    token_index = safe_owner // top_k
    slot_gates = jnp.where(
        is_used, gate_weights.reshape(-1)[safe_owner], jnp.zeros((), jnp.bfloat16)
    )
    slot_gates = slot_gates.reshape(expert_count, capacity)

    def gather_slots(source):
        picked_rows = jnp.where(is_used[:, None], source[token_index], jnp.zeros((), jnp.bfloat16))
        return picked_rows.reshape(expert_count, capacity, source.shape[1])

    col_width = model_width // lax.axis_size("tp")
    col_start = lax.axis_index("tp") * col_width
    token_cols = lax.dynamic_slice_in_dim(tokens, col_start, col_width, 1)
    cot_cols = lax.dynamic_slice_in_dim(cotangent, col_start, col_width, 1)
    rows_part, cots_part, gates_in = (
        lax.all_to_all(gather_slots(token_cols), "ep", split_axis=0, concat_axis=0, tiled=True),
        lax.all_to_all(gather_slots(cot_cols), "ep", split_axis=0, concat_axis=0, tiled=True),
        lax.all_to_all(slot_gates, "ep", split_axis=0, concat_axis=0, tiled=True),
    )
    in_rows, cot_in = (
        lax.all_gather(rows_part, "tp", axis=2, tiled=True),
        lax.all_gather(cots_part, "tp", axis=2, tiled=True),
    )
    slot_count = in_rows.shape[0] * in_rows.shape[1]
    grad_in, gate_part, grad_gate, grad_upw, grad_down = expert_backward(
        in_rows.reshape(slot_count, model_width),
        cot_in.reshape(slot_count, model_width),
        gates_in.reshape(slot_count, 1).astype(jnp.float32),
        gate_proj[0],
        up_proj[0],
        down_proj[0],
    )
    gate_total = lax.psum(gate_part, "tp")
    grad_cols = lax.psum_scatter(
        grad_in.astype(jnp.bfloat16), "tp", scatter_dimension=1, tiled=True
    ).astype(jnp.float32)
    back_rows, back_gates = (
        lax.all_to_all(
            grad_cols.reshape(expert_count, capacity, grad_cols.shape[1]).astype(jnp.bfloat16),
            "ep",
            split_axis=0,
            concat_axis=0,
            tiled=True,
        ).astype(jnp.float32),
        lax.all_to_all(
            gate_total.reshape(expert_count, capacity).astype(jnp.bfloat16),
            "ep",
            split_axis=0,
            concat_axis=0,
            tiled=True,
        ).astype(jnp.float32),
    )
    picked = back_rows.reshape(expert_count * capacity, back_rows.shape[2])[slot_index]
    grad_tokens = jnp.sum(picked.reshape(tok_rows, top_k, picked.shape[1]), axis=1).astype(
        jnp.bfloat16
    )
    grad_gates = back_gates.reshape(-1)[slot_index].reshape(tok_rows, top_k)
    return (grad_tokens, grad_gates, grad_gate[None], grad_upw[None], grad_down[None])


MESH = pl.DeviceIdType.MESH


def flip(index, mask):
    if mask & 1:
        index = index + 1 - 2 * (index % 2)
    if mask & 2:
        index = index + 2 - 4 * ((index // 2) % 2)
    if mask & 4:
        index = index + 4 - 8 * ((index // 4) % 2)
    return index


class Copies:
    def __init__(self, send_sem, recv_sem):
        self.send_sem, self.recv_sem, self.made = send_sem, recv_sem, []

    def send(self, src, dst, ep, tp):
        n = len(self.made)
        copy = pltpu.make_async_remote_copy(
            src_ref=src,
            dst_ref=dst,
            send_sem=self.send_sem.at[n],
            recv_sem=self.recv_sem.at[n],
            device_id=(ep, tp),
            device_id_type=MESH,
        )
        copy.start()
        self.made.append(copy)
        return copy

    def finish(self):
        for copy in self.made:
            copy.wait_send()


def gather_kernel(tok, cot, gate, tok_out, cot_out, gate_out, send_sem, recv_sem, own_sem):
    me, t = lax.axis_index("ep"), lax.axis_index("tp")
    width = tok.shape[1]
    eighth = width // 8
    quarter = 2 * eighth
    q, far = t % 4, flip(t % 4, 2)

    def cols(start, size):
        return pl.ds(pl.multiple_of(start, 128), size)

    low, high = cols(quarter * q, eighth), cols(quarter * q + eighth, eighth)
    full = cols(quarter * q, quarter)
    far_low, far_high = cols(quarter * far, eighth), cols(quarter * far + eighth, eighth)
    far_full = cols(quarter * far, quarter)
    pairs = ((tok, tok_out), (cot, cot_out))
    own = [
        pltpu.make_async_copy(src, dst.at[0], own_sem.at[a]) for a, (src, dst) in enumerate(pairs)
    ]
    for copy in own:
        copy.start()
    do = Copies(send_sem, recv_sem)
    gates = [do.send(gate.at[j], gate_out.at[j], flip(me, j), t) for j in (1, 2, 3)]
    relayed, direct = [], []
    for src, dst in pairs:
        for j, where in ((3, full), (1, high), (2, high)):
            copy = do.send(src.at[:, where], dst.at[j, :, where], flip(me, j), t)
            relayed.append((copy, dst, j, where))
    for src, dst in pairs:
        for where in (low, far_low):
            for j in (1, 2):
                copy = do.send(src.at[:, where], dst.at[j, :, where], flip(me, j), t)
                direct.append((copy, dst, j, where))
    last = []
    for copy, dst, j, where in relayed:
        copy.wait_recv()
        piece = dst.at[j, :, where]
        moved = do.send(piece, piece, me, flip(t, 2))
        direct.append((moved, dst, j, far_full if j == 3 else far_high))
        last.append(do.send(piece, piece, me, flip(t, 1)))
    for copy, dst, j, where in direct:
        copy.wait_recv()
        piece = dst.at[j, :, where]
        last.append(do.send(piece, piece, me, flip(t, 1)))
    for copy in last + gates:
        copy.wait_recv()
    do.finish()
    gate_out[0] = gate[0]
    for copy in own:
        copy.wait()


def gather(tokens, cotangent, gate):
    experts = lax.axis_size("ep")
    shape = jax.ShapeDtypeStruct((experts,) + tokens.shape, tokens.dtype)
    vmem = pl.BlockSpec(memory_space=pltpu.VMEM)
    return pl.pallas_call(
        gather_kernel,
        out_shape=[shape, shape, jax.ShapeDtypeStruct(gate.shape, gate.dtype)],
        in_specs=[vmem] * 3,
        out_specs=[vmem] * 3,
        scratch_shapes=[
            pltpu.SemaphoreType.DMA((43,)),
            pltpu.SemaphoreType.DMA((43,)),
            pltpu.SemaphoreType.DMA((2,)),
        ],
        compiler_params=pltpu.CompilerParams(has_side_effects=True, vmem_limit_bytes=14 << 20),
    )(tokens, cotangent, gate)


def reduce_kernel(part, gate, out, gate_out, r1, m, r2, s, r3, rg, g, send_sem, recv_sem):
    me, t = lax.axis_index("ep"), lax.axis_index("tp")
    core, z = t % 2, t // 2
    size = out.shape[1]
    other = flip(t, 1)
    order = (3, 2, 1, 0)
    blocks = (3, 1, 2, 0)
    f32 = jnp.float32

    def cols(d, which):
        return pl.ds(pl.multiple_of((2 * flip(z, d) + which) * size, 128), size)

    do = Copies(send_sem, recv_sem)
    first = {}
    for d in order:
        for j in blocks:
            first[d, j] = do.send(part.at[j, :, cols(d, 1 - core)], r1.at[d, j], me, other)
        if d == 3:
            stage = do.send(gate, rg.at[0], me, other)
    second = {}
    for n, d in enumerate(order):
        for j in blocks:
            first[d, j].wait_recv()
            mine = part[j, :, cols(d, core)].astype(f32)
            m[d, j] = (mine + r1[d, j].astype(f32)).astype(m.dtype)
            if j > 0:
                second[d, j] = do.send(m.at[d, j], r2.at[d, j], flip(me, j), t)
        if n < 3:
            stage.wait_recv()
            g[n] = (gate[...] if n == 0 else g[n - 1]) + rg[n]
            if n < 2:
                stage = do.send(g.at[n], rg.at[n + 1], me, flip(t, 2 << n))
    gates = [do.send(g.at[2, j], gate_out.at[j], flip(me, j), t) for j in (1, 2, 3)]
    third = {}
    for d in order:
        total = m[d, 0].astype(f32)
        for j in (1, 2, 3):
            second[d, j].wait_recv()
            total = total + r2[d, j].astype(f32)
        if d:
            s[d] = total.astype(s.dtype)
            third[d] = do.send(s.at[d], r3.at[d], me, flip(t, 2 * d))
    for d in (3, 2, 1):
        third[d].wait_recv()
        total = total + r3[d].astype(f32)
    out[...] = total.astype(out.dtype)
    for copy in gates:
        copy.wait_recv()
    do.finish()
    gate_out[0] = g[2, 0]


def reduce(part, gate):
    experts, parts = lax.axis_size("ep"), lax.axis_size("tp")
    rows, size = part.shape[1], part.shape[2] // parts
    vmem = pl.BlockSpec(memory_space=pltpu.VMEM)
    slots = parts // 2
    tile = pltpu.VMEM((slots, experts, rows, size), part.dtype)
    return pl.pallas_call(
        reduce_kernel,
        out_shape=[
            jax.ShapeDtypeStruct((rows, size), part.dtype),
            jax.ShapeDtypeStruct(gate.shape, gate.dtype),
        ],
        in_specs=[vmem] * 2,
        out_specs=[vmem] * 2,
        scratch_shapes=[
            tile,
            tile,
            tile,
            pltpu.VMEM((slots, rows, size), part.dtype),
            pltpu.VMEM((slots, rows, size), part.dtype),
            pltpu.VMEM((3,) + gate.shape, gate.dtype),
            pltpu.VMEM((3,) + gate.shape, gate.dtype),
            pltpu.SemaphoreType.DMA((37,)),
            pltpu.SemaphoreType.DMA((37,)),
        ],
        compiler_params=pltpu.CompilerParams(has_side_effects=True, vmem_limit_bytes=20 << 20),
    )(part, gate)


def tiles(values):
    rows = values.shape[1]
    padded = jnp.pad(values, ((0, 0), (0, -rows % 128)))
    return jnp.broadcast_to(padded[:, None, :], (padded.shape[0], 8, padded.shape[1]))


def dense(tokens, cotangent, routing, gate_weights, gate_proj, up_proj, down_proj):
    f32, bf16 = jnp.float32, jnp.bfloat16
    experts = lax.axis_size("ep")
    rows, width = tokens.shape
    me = lax.axis_index("ep")
    named = [routing == (me ^ j) for j in range(experts)]
    weights = jnp.stack(
        [jnp.sum(jnp.where(n, gate_weights.astype(f32), 0.0), axis=1) for n in named]
    )
    x_all, cot_all, g_all = gather(tokens, cotangent, tiles(weights))
    x, cot = x_all.reshape(-1, width), cot_all.reshape(-1, width)
    g = g_all[:, 0, :rows].reshape(-1, 1)
    grad_in, gate_part, d_gate, d_up, d_down = expert_backward(
        x, cot, g, gate_proj[0], up_proj[0], down_proj[0]
    )
    grad_tokens, gate_sum = reduce(
        grad_in.astype(bf16).reshape(experts, rows, width),
        tiles(gate_part.reshape(experts, rows)),
    )
    grad_gates = jnp.zeros(routing.shape, f32)
    for j in range(experts):
        grad_gates = jnp.where(named[j], gate_sum[j, 0, :rows][:, None], grad_gates)
    return grad_tokens, grad_gates, d_gate[None], d_up[None], d_down[None]


def local(tokens, cotangent, routing, gate_weights, gate_proj, up_proj, down_proj):
    experts, parts = lax.axis_size("ep"), lax.axis_size("tp")
    capacity = 2 * tokens.shape[0] * routing.shape[1] // experts
    fits = experts == 4 and parts == 8 and tokens.shape[1] % 1024 == 0
    plan = dense if capacity >= tokens.shape[0] and fits else slotted
    return plan(tokens, cotangent, routing, gate_weights, gate_proj, up_proj, down_proj)


def solution(mesh):
    return jax.shard_map(
        local,
        mesh=mesh,
        in_specs=(
            P("ep", None),
            P("ep", None),
            P("ep", None),
            P("ep", None),
            P("ep", None, "tp"),
            P("ep", None, "tp"),
            P("ep", "tp", None),
        ),
        out_specs=(
            P("ep", "tp"),
            P("ep", None),
            P("ep", None, "tp"),
            P("ep", None, "tp"),
            P("ep", "tp", None),
        ),
        check_vma=False,
    )
```
